128 devices in a mesh: rep: 2 (over z_hi), fs: 32 (over z_lo, y, x), tp: 2 (over core).
Axes of the slice: x: 4, y: 4, z: 4 (z_hi: 2, z_lo: 2; z = z_hi * 2 + z_lo), core: 2. Of those that a mesh axis runs over, the one named last changes fastest.
Arguments:
- tokens: bfloat16 [65536, 2048], P(('rep', 'fs'), 'tp'), may hold values from -13 to 13
- norm_gains: float32 [4, 2048], replicated, may hold values from 0.1 to 1.9
- mix_weight: float32 [2048, 2048], P('fs', 'tp'), may hold values from -0.125 to 0.125
- mix_scale: float32 [32, 64], P('tp', 'fs'), may hold values from 0.5 to 2
- group_weight: float32 [4, 512, 512], P('tp', 'fs'), may hold values from -0.25 to 0.25
- group_scale: float32 [32, 64], P('tp', 'fs'), may hold values from 0.35 to 2.9
- up_weight: float32 [2048, 4096], P('fs', 'tp'), may hold values from -0.125 to 0.125
- up_scale: float32 [64, 64], P('tp', 'fs'), may hold values from 0.5 to 2
- down_weight: float32 [4096, 2048], P('tp', 'fs'), may hold values from -0.09375 to 0.09375
- down_scale: float32 [32, 64], P('tp', 'fs'), may hold values from 0.35 to 2.9
Outputs:
- layer_out: bfloat16 [65536, 2048], P(('rep', 'fs'), 'tp')
The draws below stay inside these ranges and needn't reach their ends.
All inputs are finite; a program needn't handle non-finite values.
Results may differ from the reference program's by a relative error of at most 0.0083.
Values may be sent and summed in bfloat16 or wider, within the bound.
No kernel may reach another device: no remote copies, remote signals or barrier semaphores. Data moves between devices by JAX's collectives and lax.ppermute only.
A program may use at most 128 MiB of HBM per device.

```python
import math
import jax
import jax.numpy as jnp
from jax import lax

D = 2048
GROUPS = 4
GW = 512
FF = 4096
LENGTH = 1024
TOKENS = 65536
N_TP = 2


def draw_tokens(key, part):
    noise_key, column_key = jax.random.split(jax.random.fold_in(key, 11))
    base = jnp.clip(jax.random.normal(noise_key, (TOKENS, D), jnp.float32), -4.0, 4.0)
    column = 10.0 ** jax.random.uniform(column_key, (1, D), jnp.float32, -0.5, 0.5)
    return (base * column).astype(jnp.bfloat16)


def ramp_scale(key, height):
    spread = 10.0 ** jax.random.uniform(key, (height, 64), jnp.float32, -0.15, 0.15)
    rising = 4.0 ** (jnp.arange(height, dtype=jnp.float32)[:, None] / (height - 1) - 0.5)
    return spread * rising


def draw_group_scale(key, part):
    return ramp_scale(jax.random.fold_in(key, 21), D // 64)


def draw_down_scale(key, part):
    return ramp_scale(jax.random.fold_in(key, 31), D // 64)


def level_of(stream_key, dims, shards, low, high):
    gain, own = 1.0, jax.random.fold_in(stream_key, 6)
    for dim, parts in shards:
        steps = jnp.exp(jax.random.uniform(jax.random.fold_in(own, dim), (parts,), jnp.float32, low / len(shards), high / len(shards)))
        gain = gain * jnp.repeat(steps, dims[dim] // parts).reshape([-1 if axis == dim else 1 for axis in range(len(dims))])
    return gain


def bell_draw(rng, dims, width, limit, shards=(), kind=jnp.bfloat16):
    values = jax.random.normal(rng, dims, jnp.float32) * width
    if len(shards) > 0:
        values = level_of(rng, dims, shards, -0.22, 0.18) * values
    return jnp.clip(values, min=-limit, max=limit).astype(kind)


def setup_inputs(seed: int = 0) -> dict:
    key_of = jax.random.split(jax.random.key(seed), 11)
    return {
        "tokens": draw_tokens(jax.random.fold_in(key_of[10], 71), 0),
        "norm_gains": jnp.clip(1.0 + 0.18 * jax.random.normal(key_of[1], (4, D), jnp.float32), 0.1, 1.9),
        "mix_weight": bell_draw(key_of[2], (D, D), D ** -0.5, 0.125, ((0, 32), (1, 2)), jnp.float32),
        "mix_scale": jnp.clip(jnp.exp(math.log(2.0) - 1.3862944 * jax.random.uniform(key_of[3], (D // 64, 64), jnp.float32) ** level_of(key_of[3], (D // 64, 64), ((0, 2), (1, 32)), -0.2, 0.2)), 0.5, 2.0),
        "group_weight": bell_draw(key_of[4], (GROUPS, GW, GW), GW ** -0.5, 0.25, ((0, 2), (1, 32)), jnp.float32),
        "group_scale": draw_group_scale(jax.random.fold_in(key_of[10], 71), 0),
        "up_weight": bell_draw(key_of[6], (D, FF), D ** -0.5, 0.125, ((0, 32), (1, 2)), jnp.float32),
        "up_scale": jnp.clip(jnp.exp(math.log(2.0) - 1.3862944 * jax.random.uniform(key_of[7], (FF // 64, 64), jnp.float32) ** level_of(key_of[7], (FF // 64, 64), ((0, 2), (1, 32)), -0.2, 0.2)), 0.5, 2.0),
        "down_weight": bell_draw(key_of[8], (FF, D), FF ** -0.5, 0.09375, ((0, 2), (1, 32)), jnp.float32),
        "down_scale": draw_down_scale(jax.random.fold_in(key_of[10], 71), 0),
    }


epsilon = 1e-06

def rounded(values):
    return lax.optimization_barrier(values.astype(jnp.bfloat16)).astype(jnp.float32)

def inverse_rms(values):
    return lax.rsqrt(lax.optimization_barrier(jnp.mean(values * values, axis=1, keepdims=True)) + epsilon)

def pool_groups(mixed):
    length = mixed.shape[0]
    upward = mixed.astype(jnp.float32).reshape(length, GROUPS, GW)
    sums = jnp.concatenate([jnp.zeros((17, GROUPS, GW), jnp.float32), jnp.cumsum(upward, axis=0)], axis=0)
    position = jnp.arange(length, dtype=jnp.int32)
    pieces = []
    for group in range(GROUPS):
        window = 2 ** (group + 1)
        upper = sums[17:, group]
        lower = sums[17 - window:17 - window + length, group]
        count = jnp.minimum(position + 1, window).astype(jnp.float32)[:, None]
        pieces.append((upper - lower) / count - upward[:, group])
    return jnp.stack(pieces, axis=1).astype(jnp.bfloat16)

def reference(tokens, norm_gains, mix_weight, mix_scale, group_weight, group_scale, up_weight, up_scale, down_weight, down_scale):
    mix_matrix = mix_weight.astype(jnp.bfloat16)
    group_matrix = group_weight.astype(jnp.bfloat16).astype(jnp.float32)
    up_matrix = up_weight.astype(jnp.bfloat16)
    down_matrix = down_weight.astype(jnp.bfloat16)
    mix_cols = mix_scale.reshape(-1)
    group_cols = group_scale.reshape(-1)
    up_cols = up_scale.reshape(-1)
    down_cols = down_scale.reshape(-1)
    block = FF // N_TP

    def one_sequence(sequence):
        seq_float = sequence.astype(jnp.float32)
        normed = (seq_float * inverse_rms(seq_float) * norm_gains[0]).astype(jnp.bfloat16)
        mixed = (jnp.dot(normed, mix_matrix, preferred_element_type=jnp.float32) * mix_cols).astype(jnp.bfloat16)
        pooled = pool_groups(mixed)
        grouped = jnp.einsum('sgc,gcd->sgd', pooled.astype(jnp.float32), group_matrix).reshape(LENGTH, D)
        branch = rounded(grouped * group_cols)
        middle = (seq_float + rounded(branch * inverse_rms(branch) * norm_gains[1])).astype(jnp.bfloat16)
        mid_float = middle.astype(jnp.float32)
        normed_mid = (mid_float * inverse_rms(mid_float) * norm_gains[2]).astype(jnp.bfloat16)
        upward = jnp.dot(normed_mid, up_matrix, preferred_element_type=jnp.float32) * up_cols
        active = jnp.maximum(upward, 0.0)
        hidden = (active * active).astype(jnp.bfloat16)
        total = jnp.zeros((LENGTH, D), jnp.float32)
        for shard in range(N_TP):
            partial_term = jnp.dot(hidden[:, shard * block:(shard + 1) * block], down_matrix[shard * block:(shard + 1) * block], preferred_element_type=jnp.float32)
            total = total + rounded(partial_term)
        down = rounded(total * down_cols)
        return (mid_float + rounded(down * inverse_rms(down) * norm_gains[3])).astype(jnp.bfloat16)
    result = lax.map(one_sequence, tokens.reshape(-1, LENGTH, D))
    return result.reshape(-1, D)
```

```python
import functools
import jax
import jax.numpy as jnp
from jax import lax
from jax.experimental import pallas as pl
from jax.experimental.pallas import tpu as pltpu
from jax.sharding import Mesh
from jax.sharding import PartitionSpec as P

FS = ("fs_0", "fs_1", "fs_2")
REP_FS = ("rep", "fs_0", "fs_1", "fs_2")
EVERY = REP_FS + ("tp",)

EPS = 1e-06
F32, BF16 = jnp.float32, jnp.bfloat16
MIB = 1 << 20

PAIRING = (1, 3, 4, 12, 16, 48)

MIX_ORDERS = ((0, 2, 4, 1, 3), (2, 0, 5, 3, 1), (1, 3, 2, 0, 4), (3, 1, 0, 2, 5))
UP_ORDERS = ((0, 4, 3, 2, 1), (2, 5, 1, 0, 3), (1, 2, 0, 3, 4), (3, 0, 2, 1, 5))
DOWN_ORDERS = ((3, 1, 4, 2, 0), (1, 3, 5, 0, 2), (2, 1, 3, 0, 4), (0, 3, 1, 2, 5))
UP_WIDTHS = (512, 512, 512, 512)
DOWN_WIDTHS = (512, 512, 512, 512)


def swap_tp(x):
    return lax.ppermute(x, "tp", [(0, 1), (1, 0)])


def swap_with(x, way):
    return lax.ppermute(x, REP_FS, [(i, i ^ PAIRING[way]) for i in range(64)])


def gathered(x, order):
    for way in order[:-1]:
        x = jnp.concatenate([x, swap_with(x, way)], axis=0)
    return x, swap_with(x, order[-1])


def source_mask(order, place):
    mask = 0
    for k, way in enumerate(order):
        if (place >> k) & 1:
            mask ^= PAIRING[way] & 31
    return mask


def pieces_of(refs, order, rows):
    half = 1 << (len(order) - 1)
    for place in range(2 * half):
        ref = refs[0] if place < half else refs[1]
        yield ref, (place % half) * rows, source_mask(order, place)


def mix_kernel(where, normed, mix_cols, group_cols, *refs):
    n = len(MIX_ORDERS)
    chunks, (out, w, g, m, w_sems, g_sems) = refs[: 2 * n], refs[2 * n :]
    fs, tp = where[0], where[1]
    for j, order in enumerate(MIX_ORDERS):
        for ref, row, mask in pieces_of(chunks[2 * j : 2 * j + 2], order, 80):
            at = pl.multiple_of((fs ^ (tp * 16) ^ mask) * 64, 64)
            pltpu.make_async_copy(
                ref.at[pl.ds(row, 64), :],
                w.at[pl.ds(at, 64), pl.ds(j * 256, 256)],
                w_sems.at[j],
            ).start()
            at = pl.multiple_of((fs ^ mask) * 16, 16)
            pltpu.make_async_copy(
                ref.at[pl.ds(row + 64, 16), :],
                g.at[j // 2, pl.ds(at, 16), pl.ds((j % 2) * 256, 256)],
                g_sems.at[j],
            ).start()
    m[0:16, :] = jnp.zeros((16, 1024), F32)
    for j in range(n):
        here = w.at[:, pl.ds(j * 256, 256)]
        pltpu.make_async_copy(here, here, w_sems.at[j]).wait()
        here = g.at[j // 2, :, pl.ds((j % 2) * 256, 256)]
        pltpu.make_async_copy(here, here, g_sems.at[j]).wait()
    rows = 256
    for b in range(1024 // rows):
        left = normed[b * rows : (b + 1) * rows, :]
        for k in range(2):
            cols = slice(k * 512, (k + 1) * 512)
            mixed = jnp.dot(left, w[:, cols], preferred_element_type=F32)
            mixed = (mixed * mix_cols[:, cols]).astype(BF16).astype(F32)
            m[16 + b * rows : 16 + (b + 1) * rows, cols] = mixed
            x = m[b * rows : 16 + (b + 1) * rows, cols]
            two = x + pltpu.roll(x, 1, 0)
            four = two + pltpu.roll(two, 2, 0)
            eight = four + pltpu.roll(four, 4, 0)
            if k == 0:
                sums = jnp.where(tp == 0, two, eight)
                window = jnp.where(tp == 0, 2, 8)
            else:
                sums = jnp.where(tp == 0, four, eight + pltpu.roll(eight, 8, 0))
                window = jnp.where(tp == 0, 4, 16)
            t = lax.broadcasted_iota(jnp.int32, (rows, 1), 0) + (b * rows + 1)
            count = jnp.minimum(t, window).astype(F32)
            pooled = (sums[16:] * (1.0 / count) - mixed).astype(BF16)
            grouped = jnp.dot(pooled, g[k], preferred_element_type=F32)
            out[b * rows : (b + 1) * rows, cols] = (grouped * group_cols[:, cols]).astype(BF16)


def middle_kernel(tok_a, tok_b, br_a, br_b, gain_1, gain_2, mid, normed):
    rows = 128

    @pl.loop(0, 1024 // rows)
    def _(b):
        r = pl.ds(pl.multiple_of(b * rows, rows), rows)
        x, y = br_a[r, :].astype(F32), br_b[r, :].astype(F32)
        square = jnp.sum(x * x, axis=1, keepdims=True) + jnp.sum(y * y, axis=1, keepdims=True)
        inverse = lax.rsqrt(square * (1.0 / 2048) + EPS)
        x = (x * inverse * gain_1[:, :1024]).astype(BF16).astype(F32)
        y = (y * inverse * gain_1[:, 1024:]).astype(BF16).astype(F32)
        x = (tok_a[r, :].astype(F32) + x).astype(BF16)
        y = (tok_b[r, :].astype(F32) + y).astype(BF16)
        mid[r, :] = x
        x, y = x.astype(F32), y.astype(F32)
        square = jnp.sum(x * x, axis=1, keepdims=True) + jnp.sum(y * y, axis=1, keepdims=True)
        inverse = lax.rsqrt(square * (1.0 / 2048) + EPS)
        normed[r, :1024] = (x * inverse * gain_2[:, :1024]).astype(BF16)
        normed[r, 1024:] = (y * inverse * gain_2[:, 1024:]).astype(BF16)


def up_kernel(where, normed, up_cols, *refs):
    n = len(UP_ORDERS)
    chunks, (out, w, sems) = refs[: 2 * n], refs[2 * n :]
    fs, tp = where[0], where[1]
    starts = [sum(UP_WIDTHS[:j]) for j in range(n)]
    for j, order in enumerate(UP_ORDERS):
        for ref, row, mask in pieces_of(chunks[2 * j : 2 * j + 2], order, 64):
            at = pl.multiple_of((fs ^ (tp * 16) ^ mask) * 64, 64)
            pltpu.make_async_copy(
                ref.at[pl.ds(row, 64), :],
                w.at[pl.ds(at, 64), pl.ds(starts[j], UP_WIDTHS[j])],
                sems.at[j],
            ).start()
    rows = 256
    for j in range(n):
        cols = slice(starts[j], starts[j] + UP_WIDTHS[j])
        here = w.at[:, pl.ds(starts[j], UP_WIDTHS[j])]
        pltpu.make_async_copy(here, here, sems.at[j]).wait()
        for b in range(1024 // rows):
            upward = jnp.dot(
                normed[b * rows : (b + 1) * rows, :], w[:, cols], preferred_element_type=F32
            )
            active = jnp.maximum(upward * up_cols[:, cols], 0.0)
            out[b * rows : (b + 1) * rows, cols] = (active * active).astype(BF16)


NT = (((1,), (1,)), ((), ()))


def down_kernel(where, hid_a, hid_b, down_cols, *refs):
    n = len(DOWN_ORDERS)
    chunks, (out, square, w, sems) = refs[: 2 * n], refs[2 * n :]
    fs, tp = where[0], where[1]
    starts = [sum(DOWN_WIDTHS[:j]) for j in range(n)]
    for j, order in enumerate(DOWN_ORDERS):
        for ref, row, mask in pieces_of(chunks[2 * j : 2 * j + 2], order, 64):
            at = pl.multiple_of((fs ^ (tp * 16) ^ mask) * 64, 64)
            pltpu.make_async_copy(
                ref.at[pl.ds(row, 64), :],
                w.at[pl.ds(at, 64), pl.ds(starts[j], DOWN_WIDTHS[j])],
                sems.at[j],
            ).start()
    for j in range(n):
        here = w.at[:, pl.ds(starts[j], DOWN_WIDTHS[j])]
        pltpu.make_async_copy(here, here, sems.at[j]).wait()
    rows = 256
    for b in range(1024 // rows):
        r = slice(b * rows, (b + 1) * rows)
        squares = jnp.zeros((rows, 1), F32)
        for k in range(2):
            cols = slice(k * 512, (k + 1) * 512)
            total = lax.dot_general(hid_a[r, :], w[k * 512 : (k + 1) * 512, :], NT, preferred_element_type=F32)
            total += lax.dot_general(
                hid_b[r, :], w[1024 + k * 512 : 1024 + (k + 1) * 512, :], NT, preferred_element_type=F32
            )
            down = (total * down_cols[:, cols]).astype(BF16)
            out[r, cols] = down
            down = down.astype(F32)
            squares += jnp.sum(down * down, axis=1, keepdims=True)
        square[r, :] = squares


SMEM = pl.BlockSpec(memory_space=pltpu.SMEM)
VMEM = pl.BlockSpec(memory_space=pltpu.VMEM)
ANY = pl.BlockSpec(memory_space=pl.ANY)


def call(kernel, name, out_shape, in_specs, scratch, limit, flops):
    multiple = isinstance(out_shape, tuple)
    return pl.pallas_call(
        kernel,
        name=name,
        out_shape=out_shape,
        in_specs=in_specs,
        out_specs=(VMEM,) * len(out_shape) if multiple else VMEM,
        scratch_shapes=scratch,
        compiler_params=pltpu.CompilerParams(vmem_limit_bytes=limit * MIB),
        cost_estimate=pl.CostEstimate(flops=flops, bytes_accessed=16 * MIB, transcendentals=0),
    )


def shape(*dims, dtype=BF16):
    return jax.ShapeDtypeStruct(dims, dtype)


def on_device(
    tokens,
    norm_gains,
    mix_weight,
    mix_scale,
    group_weight,
    group_scale,
    up_weight,
    up_scale,
    down_weight,
    down_scale,
):
    tp = lax.axis_index("tp")
    fs = lax.axis_index(FS)
    where = jnp.stack([fs, tp]).astype(jnp.int32)
    half = 1024

    mix, group = mix_weight.astype(BF16), group_weight.astype(BF16)
    mix_parts = []
    for j, order in enumerate(MIX_ORDERS):
        cols = slice((j % 2) * 256, (j % 2) * 256 + 256)
        part = jnp.concatenate([mix[:, j * 256 : (j + 1) * 256], group[j // 2, :, cols]], axis=0)
        mix_parts += gathered(part, order)

    other = swap_tp(tokens)

    scales = jnp.concatenate([s.reshape(-1) for s in (mix_scale, group_scale, up_scale, down_scale)])
    scales = lax.all_to_all(
        jnp.broadcast_to(scales, (32, 1, 160)), FS, split_axis=0, concat_axis=0, tiled=True
    ).reshape(32, 80, 2)
    scales = jnp.transpose(scales, (1, 0, 2)).reshape(80, 64)
    mix_cols = scales[:16].reshape(1, -1)
    group_cols = scales[16:32].reshape(1, -1)
    up_cols = scales[32:64].reshape(1, -1)
    down_cols = scales[64:].reshape(1, -1)

    gains = norm_gains.reshape(4, 2, half)
    gains = jnp.where(tp == 0, gains, gains[:, ::-1]).reshape(4, 2 * half)

    a, b = tokens.astype(F32), other.astype(F32)
    square = jnp.sum(a * a, axis=1, keepdims=True) + jnp.sum(b * b, axis=1, keepdims=True)
    inverse = lax.rsqrt(square / (2 * half) + EPS)
    normed = jnp.concatenate(
        [
            (a * inverse * gains[:1, :half]).astype(BF16),
            (b * inverse * gains[:1, half:]).astype(BF16),
        ],
        axis=1,
    )

    up = up_weight.astype(BF16)
    up_parts = []
    at = 0
    for width, order in zip(UP_WIDTHS, UP_ORDERS):
        up_parts += gathered(up[:, at : at + width], order)
        at += width

    down = jnp.transpose(down_weight.astype(BF16))
    trade = []
    for i in range(64):
        for c in range(2):
            trade.append((i * 2 + c, i * 2 + c if (i >> 4) & 1 == c else (i ^ 16) * 2 + 1 - c))
    down = lax.ppermute(down, EVERY, trade)
    down_parts = []
    at = 0
    for width, order in zip(DOWN_WIDTHS, DOWN_ORDERS):
        down_parts += gathered(down[:, at : at + width], order)
        at += width

    branch = call(
        mix_kernel,
        "mix",
        shape(1024, half),
        [SMEM, VMEM, VMEM, VMEM] + [ANY] * len(mix_parts),
        [
            pltpu.VMEM((2048, 1024), BF16),
            pltpu.VMEM((2, 512, 512), BF16),
            pltpu.VMEM((1040, 1024), F32),
            pltpu.SemaphoreType.DMA((len(MIX_ORDERS),)),
            pltpu.SemaphoreType.DMA((len(MIX_ORDERS),)),
        ],
        24,
        6 * 10**9,
    )(where, normed, mix_cols, group_cols, *mix_parts)

    middle, normed_mid = call(
        middle_kernel,
        "middle",
        (shape(1024, half), shape(1024, 2 * half)),
        [VMEM] * 6,
        [],
        20,
        10**9,
    )(tokens, other, branch, swap_tp(branch), gains[1:2], gains[2:3])

    hidden = call(
        up_kernel,
        "up",
        shape(1024, 2048),
        [SMEM, VMEM, VMEM] + [ANY] * len(up_parts),
        [pltpu.VMEM((2048, 2048), BF16), pltpu.SemaphoreType.DMA((len(UP_ORDERS),))],
        24,
        9 * 10**9,
    )(where, normed_mid, up_cols, *up_parts)

    down, square = call(
        down_kernel,
        "down",
        (shape(1024, half), shape(1024, 1, dtype=F32)),
        [SMEM, VMEM, VMEM, VMEM] + [ANY] * len(down_parts),
        [pltpu.VMEM((2048, 2048), BF16), pltpu.SemaphoreType.DMA((len(DOWN_ORDERS),))],
        30,
        9 * 10**9,
    )(where, hidden, swap_tp(hidden), down_cols, *down_parts)

    inverse = lax.rsqrt((square + swap_tp(square)) / (2 * half) + EPS)
    last = lax.reduce_precision(down.astype(F32) * inverse * gains[3:4, :half], 8, 7)
    return (middle.astype(F32) + last).astype(BF16)


def solution(mesh):
    finer = Mesh(
        mesh.devices.reshape(mesh.shape["rep"], 2, 4, 4, mesh.shape["tp"]),
        ("rep", "fs_0", "fs_1", "fs_2", "tp"),
    )
    in_specs = (
        P(REP_FS, "tp"),
        P(),
        P(FS, "tp"),
        P("tp", FS),
        P("tp", FS, None),
        P("tp", FS),
        P(FS, "tp"),
        P("tp", FS),
        P("tp", FS),
        P("tp", FS),
    )
    out_specs = P(REP_FS, "tp")
    return jax.shard_map(
        on_device, mesh=finer, in_specs=in_specs, out_specs=out_specs, check_vma=False
    )
```

```python
import functools
import jax
import jax.numpy as jnp
from jax import lax
from jax.experimental import pallas as pl
from jax.experimental.pallas import tpu as pltpu
from jax.sharding import Mesh
from jax.sharding import PartitionSpec as P

FS = ("fs_0", "fs_1", "fs_2")
REP_FS = ("rep", "fs_0", "fs_1", "fs_2")
EVERY = REP_FS + ("tp",)

EPS = 1e-06
F32, BF16 = jnp.float32, jnp.bfloat16
MIB = 1 << 20

PAIRING = (1, 3, 4, 12, 16, 48)

MIX_ORDERS = ((0, 2, 4, 1, 3), (2, 0, 5, 3, 1), (1, 3, 2, 0, 4), (3, 1, 0, 2, 5))

def swap_tp(x):
    return lax.ppermute(x, "tp", [(0, 1), (1, 0)])


def swap_with(x, way):
    return lax.ppermute(x, REP_FS, [(i, i ^ PAIRING[way]) for i in range(64)])


def gathered(x, order):
    for way in order[:-1]:
        x = jnp.concatenate([x, swap_with(x, way)], axis=0)
    return x, swap_with(x, order[-1])


def source_mask(order, place):
    mask = 0
    for k, way in enumerate(order):
        if (place >> k) & 1:
            mask ^= PAIRING[way] & 31
    return mask


def pieces_of(refs, order, rows):
    half = 1 << (len(order) - 1)
    for place in range(2 * half):
        ref = refs[0] if place < half else refs[1]
        yield ref, (place % half) * rows, source_mask(order, place)


def mix_kernel(where, normed, mix_cols, group_cols, *refs):
    n = len(MIX_ORDERS)
    chunks, (out, w, g, m, w_sems, g_sems) = refs[: 2 * n], refs[2 * n :]
    fs, tp = where[0], where[1]
    for j, order in enumerate(MIX_ORDERS):
        for ref, row, mask in pieces_of(chunks[2 * j : 2 * j + 2], order, 80):
            at = pl.multiple_of((fs ^ (tp * 16) ^ mask) * 64, 64)
            pltpu.make_async_copy(
                ref.at[pl.ds(row, 64), :],
                w.at[pl.ds(at, 64), pl.ds(j * 256, 256)],
                w_sems.at[j],
            ).start()
            at = pl.multiple_of((fs ^ mask) * 16, 16)
            pltpu.make_async_copy(
                ref.at[pl.ds(row + 64, 16), :],
                g.at[j // 2, pl.ds(at, 16), pl.ds((j % 2) * 256, 256)],
                g_sems.at[j],
            ).start()
    m[0:16, :] = jnp.zeros((16, 1024), F32)
    for j in range(n):
        here = w.at[:, pl.ds(j * 256, 256)]
        pltpu.make_async_copy(here, here, w_sems.at[j]).wait()
        here = g.at[j // 2, :, pl.ds((j % 2) * 256, 256)]
        pltpu.make_async_copy(here, here, g_sems.at[j]).wait()
    rows = 256
    for b in range(1024 // rows):
        left = normed[b * rows : (b + 1) * rows, :]
        for k in range(2):
            cols = slice(k * 512, (k + 1) * 512)
            mixed = jnp.dot(left, w[:, cols], preferred_element_type=F32)
            mixed = (mixed * mix_cols[:, cols]).astype(BF16).astype(F32)
            m[16 + b * rows : 16 + (b + 1) * rows, cols] = mixed
            x = m[b * rows : 16 + (b + 1) * rows, cols]
            two = x + pltpu.roll(x, 1, 0)
            four = two + pltpu.roll(two, 2, 0)
            eight = four + pltpu.roll(four, 4, 0)
            if k == 0:
                sums = jnp.where(tp == 0, two, eight)
                window = jnp.where(tp == 0, 2, 8)
            else:
                sums = jnp.where(tp == 0, four, eight + pltpu.roll(eight, 8, 0))
                window = jnp.where(tp == 0, 4, 16)
            t = lax.broadcasted_iota(jnp.int32, (rows, 1), 0) + (b * rows + 1)
            count = jnp.minimum(t, window).astype(F32)
            pooled = (sums[16:] * (1.0 / count) - mixed).astype(BF16)
            grouped = jnp.dot(pooled, g[k], preferred_element_type=F32)
            out[b * rows : (b + 1) * rows, cols] = (grouped * group_cols[:, cols]).astype(BF16)


def middle_kernel(tok_a, tok_b, br_a, br_b, gain_1, gain_2, mid, normed):
    rows = 128

    @pl.loop(0, 1024 // rows)
    def _(b):
        r = pl.ds(pl.multiple_of(b * rows, rows), rows)
        x, y = br_a[r, :].astype(F32), br_b[r, :].astype(F32)
        square = jnp.sum(x * x, axis=1, keepdims=True) + jnp.sum(y * y, axis=1, keepdims=True)
        inverse = lax.rsqrt(square * (1.0 / 2048) + EPS)
        x = (x * inverse * gain_1[:, :1024]).astype(BF16).astype(F32)
        y = (y * inverse * gain_1[:, 1024:]).astype(BF16).astype(F32)
        x = (tok_a[r, :].astype(F32) + x).astype(BF16)
        y = (tok_b[r, :].astype(F32) + y).astype(BF16)
        mid[r, :] = x
        x, y = x.astype(F32), y.astype(F32)
        square = jnp.sum(x * x, axis=1, keepdims=True) + jnp.sum(y * y, axis=1, keepdims=True)
        inverse = lax.rsqrt(square * (1.0 / 2048) + EPS)
        normed[r, :1024] = (x * inverse * gain_2[:, :1024]).astype(BF16)
        normed[r, 1024:] = (y * inverse * gain_2[:, 1024:]).astype(BF16)


def up_kernel(where, normed, up_cols, both, out, w, sems):
    tp = where[1]
    for i in range(64):
        at = pl.multiple_of(((i & 31) ^ (tp * 16)) * 64, 64)
        pltpu.make_async_copy(
            both.at[pl.ds(i * 128, 64), :],
            w.at[i >> 5, pl.ds(at, 64), :],
            sems.at[i >> 5],
        ).start()
    rows = 256
    for j in range(2):
        pltpu.make_async_copy(w.at[j], w.at[j], sems.at[j]).wait()
        for k in range(2):
            cols = slice(j * 1024 + k * 512, j * 1024 + k * 512 + 512)
            right = w[j, :, k * 512 : (k + 1) * 512]

            @pl.loop(0, 1024 // rows)
            def _(b):
                r = pl.ds(pl.multiple_of(b * rows, rows), rows)
                upward = jnp.dot(normed[r, :], right, preferred_element_type=F32)
                active = jnp.maximum(upward * up_cols[:, cols], 0.0)
                out[r, cols] = (active * active).astype(BF16)


NT = (((1,), (1,)), ((), ()))


def down_kernel(where, hid_a, hid_b, down_cols, both, out, square, w, sems):
    tp = where[1]
    for i in sorted(range(64), key=lambda i: (i >> 3) & 1):
        n = i & 15
        pltpu.make_async_copy(
            both.at[pl.ds(i * 128 + 64, 64), :],
            w.at[n >> 3, ((i >> 4) & 1) ^ tp, pl.ds((n & 7) * 64, 64), pl.ds((i >> 5) * 1024, 1024)],
            sems.at[n >> 3],
        ).start()
    rows = 256
    for k in range(2):
        pltpu.make_async_copy(w.at[k], w.at[k], sems.at[k]).wait()
        cols = slice(k * 512, (k + 1) * 512)

        @pl.loop(0, 1024 // rows)
        def _(b):
            r = pl.ds(pl.multiple_of(b * rows, rows), rows)
            total = lax.dot_general(hid_a[r, :], w[k, 0], NT, preferred_element_type=F32)
            total += lax.dot_general(hid_b[r, :], w[k, 1], NT, preferred_element_type=F32)
            down = (total * down_cols[:, cols]).astype(BF16)
            out[r, cols] = down
            down = down.astype(F32)
            squares = jnp.sum(down * down, axis=1, keepdims=True)
            if k == 0:
                square[r, :] = squares
            else:
                square[r, :] += squares


SMEM = pl.BlockSpec(memory_space=pltpu.SMEM)
VMEM = pl.BlockSpec(memory_space=pltpu.VMEM)
ANY = pl.BlockSpec(memory_space=pl.ANY)


def call(kernel, name, out_shape, in_specs, scratch, limit, flops):
    multiple = isinstance(out_shape, tuple)
    return pl.pallas_call(
        kernel,
        name=name,
        out_shape=out_shape,
        in_specs=in_specs,
        out_specs=(VMEM,) * len(out_shape) if multiple else VMEM,
        scratch_shapes=scratch,
        compiler_params=pltpu.CompilerParams(vmem_limit_bytes=limit * MIB),
        cost_estimate=pl.CostEstimate(flops=flops, bytes_accessed=16 * MIB, transcendentals=0),
    )


def shape(*dims, dtype=BF16):
    return jax.ShapeDtypeStruct(dims, dtype)


def on_device(
    tokens,
    norm_gains,
    mix_weight,
    mix_scale,
    group_weight,
    group_scale,
    up_weight,
    up_scale,
    down_weight,
    down_scale,
):
    tp = lax.axis_index("tp")
    fs = lax.axis_index(FS)
    where = jnp.stack([fs, tp]).astype(jnp.int32)
    half = 1024

    mix, group = mix_weight.astype(BF16), group_weight.astype(BF16)
    mix_parts = []
    for j, order in enumerate(MIX_ORDERS):
        cols = slice((j % 2) * 256, (j % 2) * 256 + 256)
        part = jnp.concatenate([mix[:, j * 256 : (j + 1) * 256], group[j // 2, :, cols]], axis=0)
        mix_parts += gathered(part, order)

    other = swap_tp(tokens)

    scales = jnp.concatenate([s.reshape(-1) for s in (mix_scale, group_scale, up_scale, down_scale)])
    scales = lax.all_to_all(
        jnp.broadcast_to(scales, (32, 1, 160)), FS, split_axis=0, concat_axis=0, tiled=True
    ).reshape(32, 80, 2)
    scales = jnp.transpose(scales, (1, 0, 2)).reshape(80, 64)
    mix_cols = scales[:16].reshape(1, -1)
    group_cols = scales[16:32].reshape(1, -1)
    up_cols = scales[32:64].reshape(1, -1)
    down_cols = scales[64:].reshape(1, -1)

    gains = norm_gains.reshape(4, 2, half)
    gains = jnp.where(tp == 0, gains, gains[:, ::-1]).reshape(4, 2 * half)

    a, b = tokens.astype(F32), other.astype(F32)
    square = jnp.sum(a * a, axis=1, keepdims=True) + jnp.sum(b * b, axis=1, keepdims=True)
    inverse = lax.rsqrt(square / (2 * half) + EPS)
    normed = jnp.concatenate(
        [
            (a * inverse * gains[:1, :half]).astype(BF16),
            (b * inverse * gains[:1, half:]).astype(BF16),
        ],
        axis=1,
    )

    down = jnp.transpose(down_weight.astype(BF16))
    trade = []
    for i in range(64):
        for c in range(2):
            trade.append((i * 2 + c, i * 2 + c if (i >> 4) & 1 == c else (i ^ 16) * 2 + 1 - c))
    down = lax.ppermute(down, EVERY, trade)
    both = jnp.concatenate([up_weight.astype(BF16), down], axis=0)
    both = lax.dynamic_slice_in_dim(both, lax.axis_index("rep") * half, half, 1)
    both = lax.all_gather(both, REP_FS, axis=0, tiled=True)

    branch = call(
        mix_kernel,
        "mix",
        shape(1024, half),
        [SMEM, VMEM, VMEM, VMEM] + [ANY] * len(mix_parts),
        [
            pltpu.VMEM((2048, 1024), BF16),
            pltpu.VMEM((2, 512, 512), BF16),
            pltpu.VMEM((1040, 1024), F32),
            pltpu.SemaphoreType.DMA((len(MIX_ORDERS),)),
            pltpu.SemaphoreType.DMA((len(MIX_ORDERS),)),
        ],
        24,
        6 * 10**9,
    )(where, normed, mix_cols, group_cols, *mix_parts)

    middle, normed_mid = call(
        middle_kernel,
        "middle",
        (shape(1024, half), shape(1024, 2 * half)),
        [VMEM] * 6,
        [],
        20,
        10**9,
    )(tokens, other, branch, swap_tp(branch), gains[1:2], gains[2:3])

    hidden = call(
        up_kernel,
        "up",
        shape(1024, 2048),
        [SMEM, VMEM, VMEM, ANY],
        [pltpu.VMEM((2, 2048, 1024), BF16), pltpu.SemaphoreType.DMA((2,))],
        50,
        9 * 10**9,
    )(where, normed_mid, up_cols, both)

    down, square = call(
        down_kernel,
        "down",
        (shape(1024, half), shape(1024, 1, dtype=F32)),
        [SMEM, VMEM, VMEM, VMEM, ANY],
        [pltpu.VMEM((2, 2, 512, 2048), BF16), pltpu.SemaphoreType.DMA((2,))],
        50,
        9 * 10**9,
    )(where, hidden, swap_tp(hidden), down_cols, both)

    inverse = lax.rsqrt((square + swap_tp(square)) / (2 * half) + EPS)
    last = lax.reduce_precision(down.astype(F32) * inverse * gains[3:4, :half], 8, 7)
    return (middle.astype(F32) + last).astype(BF16)


def solution(mesh):
    finer = Mesh(
        mesh.devices.reshape(mesh.shape["rep"], 2, 4, 4, mesh.shape["tp"]),
        ("rep", "fs_0", "fs_1", "fs_2", "tp"),
    )
    in_specs = (
        P(REP_FS, "tp"),
        P(),
        P(FS, "tp"),
        P("tp", FS),
        P("tp", FS, None),
        P("tp", FS),
        P(FS, "tp"),
        P("tp", FS),
        P("tp", FS),
        P("tp", FS),
    )
    out_specs = P(REP_FS, "tp")
    return jax.shard_map(
        on_device, mesh=finer, in_specs=in_specs, out_specs=out_specs, check_vma=False
    )
```

```python
import functools
import jax
import jax.numpy as jnp
from jax import lax
from jax.experimental import pallas as pl
from jax.experimental.pallas import tpu as pltpu
from jax.sharding import Mesh
from jax.sharding import PartitionSpec as P

FS = ("fs_0", "fs_1", "fs_2")
REP_FS = ("rep", "fs_0", "fs_1", "fs_2")
EVERY = REP_FS + ("tp",)

EPS = 1e-06
F32, BF16 = jnp.float32, jnp.bfloat16
MIB = 1 << 20

PAIRING = (1, 3, 4, 12, 16, 48)

MIX_ORDERS = ((0, 2, 4, 1, 3), (2, 0, 5, 3, 1), (1, 3, 2, 0, 4), (3, 1, 0, 2, 5))
UP_ORDERS = ((0, 4, 3, 2, 1), (2, 5, 1, 0, 3), (1, 2, 0, 3, 4), (3, 0, 2, 1, 5))
SCALE_ORDER = (0, 2, 4, 1, 3)
LAG = 1


def swap_tp(x):
    return lax.ppermute(x, "tp", [(0, 1), (1, 0)])


def swap_with(x, way):
    return lax.ppermute(x, REP_FS, [(i, i ^ PAIRING[way]) for i in range(64)])


def join_kernel(n, added, *refs):
    ins, outs = refs[: 2 * n + 2 * added], refs[2 * n + 2 * added :]
    for k in range(n):
        rows = ins[2 * k].shape[0]
        outs[k][:rows, :] = ins[2 * k][...]
        outs[k][rows:, :] = ins[2 * k + 1][...]
    if added:
        outs[n][...] = ins[2 * n][...] + ins[2 * n + 1][...]


def joined(name, pairs, added=()):
    outs = [shape(2 * a.shape[0], a.shape[1]) for a, _ in pairs]
    args = [x for pair in pairs for x in pair] + list(added)
    if added:
        outs.append(shape(*added[0].shape, dtype=F32))
    return call(
        functools.partial(join_kernel, len(pairs), len(added) // 2),
        name,
        tuple(outs),
        [VMEM] * len(args),
        [],
        12,
        10**6,
    )(*args)


def source_mask(order, place):
    mask = 0
    for k, way in enumerate(order):
        if (place >> k) & 1:
            mask ^= PAIRING[way] & 31
    return mask


def pieces_of(refs, order, rows):
    half = 1 << (len(order) - 1)
    for place in range(2 * half):
        ref = refs[0] if place < half else refs[1]
        yield ref, (place % half) * rows, source_mask(order, place)


def prepare_kernel(where, mix, group, up, mix_s, group_s, up_s, down_s, *outs):
    n = len(MIX_ORDERS)
    for j in range(n):
        outs[j][:64, :] = mix[:, j * 256 : (j + 1) * 256].astype(BF16)
        outs[j][64:, :] = group[j // 2, :, (j % 2) * 256 : (j % 2) * 256 + 256].astype(BF16)
    for j in range(len(UP_ORDERS)):
        outs[n + j][...] = up[:, j * 512 : (j + 1) * 512].astype(BF16)
    spread = outs[-1]
    row = 0
    for ref in (mix_s, group_s, up_s, down_s):
        count = ref.shape[1]
        place = lax.broadcasted_iota(jnp.int32, (count // 2, count), 0) * 2
        lane = lax.broadcasted_iota(jnp.int32, (count // 2, count), 1)
        column = lax.broadcasted_iota(jnp.int32, (count // 2, 128), 1)
        total = jnp.zeros((count // 2, 128), F32)
        for m in range(2):
            for c in range(2):
                own = jnp.where(lane == place + m, ref[c : c + 1, :], 0.0)
                own = jnp.sum(own, axis=1, keepdims=True)
                total = jnp.where(column == m * 64 + where[0] * 2 + c, own, total)
        spread[row : row + count // 2, :] = total
        row += count // 2


def down_part_kernel(where, down, out):
    at = pl.multiple_of(where[2] * 1024, 1024)
    out[...] = down[:, pl.ds(at, 1024)].astype(BF16)


def own_gain(gains, which, where, k):
    at = pl.multiple_of((where[1] ^ k) * 1024, 1024)
    return gains[which : which + 1, pl.ds(at, 1024)]


def columns(scales, start, count):
    return jnp.concatenate([scales[r : r + 1, :] for r in range(start, start + count)], axis=1)


def first_norm_kernel(where, tok_a, tok_b, gains, normed):
    rows = 128
    gain_a, gain_b = own_gain(gains, 0, where, 0), own_gain(gains, 0, where, 1)

    @pl.loop(0, 1024 // rows)
    def _(b):
        r = pl.ds(pl.multiple_of(b * rows, rows), rows)
        x, y = tok_a[r, :].astype(F32), tok_b[r, :].astype(F32)
        square = jnp.sum(x * x, axis=1, keepdims=True) + jnp.sum(y * y, axis=1, keepdims=True)
        inverse = lax.rsqrt(square * (1.0 / 2048) + EPS)
        normed[r, :1024] = (x * inverse * gain_a).astype(BF16)
        normed[r, 1024:] = (y * inverse * gain_b).astype(BF16)


def mix_kernel(where, normed, scales, *refs):
    n = len(MIX_ORDERS)
    chunks, (out, w, g, m, w_sems, g_sems) = refs[: 2 * n], refs[2 * n :]
    fs, tp = where[0], where[1]
    for j, order in enumerate(MIX_ORDERS):
        for ref, row, mask in pieces_of(chunks[2 * j : 2 * j + 2], order, 80):
            at = pl.multiple_of((fs ^ (tp * 16) ^ mask) * 64, 64)
            pltpu.make_async_copy(
                ref.at[pl.ds(row, 64), :],
                w.at[pl.ds(at, 64), pl.ds(j * 256, 256)],
                w_sems.at[j],
            ).start()
            at = pl.multiple_of((fs ^ mask) * 16, 16)
            pltpu.make_async_copy(
                ref.at[pl.ds(row + 64, 16), :],
                g.at[j // 2, pl.ds(at, 16), pl.ds((j % 2) * 256, 256)],
                g_sems.at[j],
            ).start()
    m[0:16, :] = jnp.zeros((16, 1024), F32)
    for j in range(n):
        here = w.at[:, pl.ds(j * 256, 256)]
        pltpu.make_async_copy(here, here, w_sems.at[j]).wait()
        here = g.at[j // 2, :, pl.ds((j % 2) * 256, 256)]
        pltpu.make_async_copy(here, here, g_sems.at[j]).wait()
    rows = 256
    for b in range(1024 // rows):
        left = normed[b * rows : (b + 1) * rows, :]
        for k in range(2):
            cols = slice(k * 512, (k + 1) * 512)
            mixed = jnp.dot(left, w[:, cols], preferred_element_type=F32)
            mixed = (mixed * columns(scales, 4 * k, 4)).astype(BF16).astype(F32)
            m[16 + b * rows : 16 + (b + 1) * rows, cols] = mixed
            x = m[b * rows : 16 + (b + 1) * rows, cols]
            two = x + pltpu.roll(x, 1, 0)
            four = two + pltpu.roll(two, 2, 0)
            eight = four + pltpu.roll(four, 4, 0)
            if k == 0:
                sums = jnp.where(tp == 0, two, eight)
                window = jnp.where(tp == 0, 2, 8)
            else:
                sums = jnp.where(tp == 0, four, eight + pltpu.roll(eight, 8, 0))
                window = jnp.where(tp == 0, 4, 16)
            t = lax.broadcasted_iota(jnp.int32, (rows, 1), 0) + (b * rows + 1)
            count = jnp.minimum(t, window).astype(F32)
            pooled = (sums[16:] * (1.0 / count) - mixed).astype(BF16)
            grouped = jnp.dot(pooled, g[k], preferred_element_type=F32)
            out[b * rows : (b + 1) * rows, cols] = (grouped * columns(scales, 8 + 4 * k, 4)).astype(BF16)


def middle_kernel(where, tok_a, tok_b, br_a, br_b, gains, mid, normed):
    rows = 128
    one_a, one_b = own_gain(gains, 1, where, 0), own_gain(gains, 1, where, 1)
    two_a, two_b = own_gain(gains, 2, where, 0), own_gain(gains, 2, where, 1)

    @pl.loop(0, 1024 // rows)
    def _(b):
        r = pl.ds(pl.multiple_of(b * rows, rows), rows)
        x, y = br_a[r, :].astype(F32), br_b[r, :].astype(F32)
        square = jnp.sum(x * x, axis=1, keepdims=True) + jnp.sum(y * y, axis=1, keepdims=True)
        inverse = lax.rsqrt(square * (1.0 / 2048) + EPS)
        x = (x * inverse * one_a).astype(BF16).astype(F32)
        y = (y * inverse * one_b).astype(BF16).astype(F32)
        x = (tok_a[r, :].astype(F32) + x).astype(BF16)
        y = (tok_b[r, :].astype(F32) + y).astype(BF16)
        mid[r, :] = x
        x, y = x.astype(F32), y.astype(F32)
        square = jnp.sum(x * x, axis=1, keepdims=True) + jnp.sum(y * y, axis=1, keepdims=True)
        inverse = lax.rsqrt(square * (1.0 / 2048) + EPS)
        normed[r, :1024] = (x * inverse * two_a).astype(BF16)
        normed[r, 1024:] = (y * inverse * two_b).astype(BF16)


def up_kernel(first, where, normed, scales, *refs):
    orders = UP_ORDERS[first : first + 2]
    chunks, (out, w, sems) = refs[:4], refs[4:]
    fs, tp = where[0], where[1]
    for j, order in enumerate(orders):
        for ref, row, mask in pieces_of(chunks[2 * j : 2 * j + 2], order, 64):
            at = pl.multiple_of((fs ^ (tp * 16) ^ mask) * 64, 64)
            pltpu.make_async_copy(
                ref.at[pl.ds(row, 64), :], w.at[j, pl.ds(at, 64), :], sems.at[j]
            ).start()
    rows = 256
    for j in range(2):
        pltpu.make_async_copy(w.at[j], w.at[j], sems.at[j]).wait()
        for b in range(1024 // rows):
            r = slice(b * rows, (b + 1) * rows)
            upward = jnp.dot(normed[r, :], w[j], preferred_element_type=F32)
            active = jnp.maximum(upward * columns(scales, 16 + 4 * (first + j), 4), 0.0)
            out[r, j * 512 : (j + 1) * 512] = (active * active).astype(BF16)


NT = (((1,), (1,)), ((), ()))


def down_kernel(where, a0, a1, b0, b1, scales, both, out, square, w, sems):
    tp = where[1]
    for i in sorted(range(64), key=lambda i: (i >> 3) & 1):
        n = i & 15
        pltpu.make_async_copy(
            both.at[pl.ds(i * 64, 64), :],
            w.at[n >> 3, ((i >> 4) & 1) ^ tp, i >> 5, pl.ds((n & 7) * 64, 64), :],
            sems.at[n >> 3],
        ).start()
    rows = 256
    for k in range(2):
        pltpu.make_async_copy(w.at[k], w.at[k], sems.at[k]).wait()
        cols = slice(k * 512, (k + 1) * 512)
        for b in range(1024 // rows):
            r = slice(b * rows, (b + 1) * rows)
            total = lax.dot_general(a0[r, :], w[k, 0, 0], NT, preferred_element_type=F32)
            total += lax.dot_general(a1[r, :], w[k, 0, 1], NT, preferred_element_type=F32)
            total += lax.dot_general(b0[r, :], w[k, 1, 0], NT, preferred_element_type=F32)
            total += lax.dot_general(b1[r, :], w[k, 1, 1], NT, preferred_element_type=F32)
            down = (total * columns(scales, 32 + 4 * k, 4)).astype(BF16)
            out[r, cols] = down
            down = down.astype(F32)
            squares = jnp.sum(down * down, axis=1, keepdims=True)
            if k == 0:
                square[r, :] = squares
            else:
                square[r, :] += squares


SMEM = pl.BlockSpec(memory_space=pltpu.SMEM)
VMEM = pl.BlockSpec(memory_space=pltpu.VMEM)
ANY = pl.BlockSpec(memory_space=pl.ANY)


def call(kernel, name, out_shape, in_specs, scratch, limit, flops):
    multiple = isinstance(out_shape, tuple)
    return pl.pallas_call(
        kernel,
        name=name,
        out_shape=out_shape,
        in_specs=in_specs,
        out_specs=(VMEM,) * len(out_shape) if multiple else VMEM,
        scratch_shapes=scratch,
        compiler_params=pltpu.CompilerParams(vmem_limit_bytes=limit * MIB),
        cost_estimate=pl.CostEstimate(flops=flops, bytes_accessed=16 * MIB, transcendentals=0),
    )


def shape(*dims, dtype=BF16):
    return jax.ShapeDtypeStruct(dims, dtype)


def on_device(
    tokens,
    norm_gains,
    mix_weight,
    mix_scale,
    group_weight,
    group_scale,
    up_weight,
    up_scale,
    down_weight,
    down_scale,
):
    tp = lax.axis_index("tp")
    where = jnp.stack([lax.axis_index(FS), tp, lax.axis_index("rep")]).astype(jnp.int32)
    half = 1024

    down = call(
        down_part_kernel, "down_part", shape(64, half), [SMEM, VMEM], [], 8, 10**6
    )(where, jnp.transpose(down_weight))
    trade = []
    for i in range(64):
        for c in range(2):
            trade.append((i * 2 + c, i * 2 + c if (i >> 4) & 1 == c else (i ^ 16) * 2 + 1 - c))
    down = lax.ppermute(down, EVERY, trade)
    down = lax.all_gather(down, REP_FS, axis=0, tiled=True)

    *parts, scales = call(
        prepare_kernel,
        "prepare",
        (shape(80, 256),) * 4 + (shape(64, 512),) * 4 + (shape(40, 128, dtype=F32),),
        [SMEM] + [VMEM] * 7,
        [],
        12,
        10**6,
    )(
        where,
        mix_weight,
        group_weight,
        up_weight,
        *(jnp.transpose(x) for x in (mix_scale, group_scale, up_scale, down_scale)),
    )
    mix_held, up_held = parts[:4], parts[4:]

    def step(held, orders, k):
        return [(x, swap_with(x, order[k])) for x, order in zip(held, orders)]

    other = swap_tp(tokens)
    up_at = 0
    for k in range(5):
        pairs = step(mix_held, MIX_ORDERS, k)
        sent = swap_with(scales, SCALE_ORDER[k])
        if k == 4:
            scales = scales + sent
            break
        *mix_held, scales = joined(f"join_mix_{k}", pairs, (scales, sent))
        if k >= LAG:
            up_pairs = step(up_held, UP_ORDERS, up_at)
            up_held = joined(f"join_up_{up_at}", up_pairs)
            up_at += 1
        if k + 1 >= LAG:
            mix_held, up_held = lax.optimization_barrier((mix_held, up_held))
    mix_parts = [x for pair in pairs for x in pair]
    while up_at < 4:
        up_held = joined(f"join_up_{up_at}", step(up_held, UP_ORDERS, up_at))
        up_at += 1
    up_parts = [x for pair in step(up_held, UP_ORDERS, 4) for x in pair]

    normed = call(
        first_norm_kernel, "first_norm", shape(1024, 2 * half), [SMEM] + [VMEM] * 3, [], 16, 10**9
    )(where, tokens, other, norm_gains)

    branch = call(
        mix_kernel,
        "mix",
        shape(1024, half),
        [SMEM, VMEM, VMEM] + [ANY] * len(mix_parts),
        [
            pltpu.VMEM((2048, 1024), BF16),
            pltpu.VMEM((2, 512, 512), BF16),
            pltpu.VMEM((1040, 1024), F32),
            pltpu.SemaphoreType.DMA((len(MIX_ORDERS),)),
            pltpu.SemaphoreType.DMA((len(MIX_ORDERS),)),
        ],
        24,
        6 * 10**9,
    )(where, normed, scales, *mix_parts)

    middle, normed_mid = call(
        middle_kernel,
        "middle",
        (shape(1024, half), shape(1024, 2 * half)),
        [SMEM] + [VMEM] * 5,
        [],
        20,
        10**9,
    )(where, tokens, other, branch, swap_tp(branch), norm_gains)

    hidden = []
    for first in (0, 2):
        hidden.append(
            call(
                functools.partial(up_kernel, first),
                f"up_{first}",
                shape(1024, 1024),
                [SMEM, VMEM, VMEM] + [ANY] * 4,
                [pltpu.VMEM((2, 2048, 512), BF16), pltpu.SemaphoreType.DMA((2,))],
                16,
                5 * 10**9,
            )(where, normed_mid, scales, *up_parts[2 * first : 2 * first + 4])
        )

    down, square = call(
        down_kernel,
        "down",
        (shape(1024, half), shape(1024, 1, dtype=F32)),
        [SMEM] + [VMEM] * 5 + [ANY],
        [pltpu.VMEM((2, 2, 2, 512, 1024), BF16), pltpu.SemaphoreType.DMA((2,))],
        36,
        9 * 10**9,
    )(where, *hidden, *(swap_tp(x) for x in hidden), scales, down)

    inverse = lax.rsqrt((square + swap_tp(square)) / (2 * half) + EPS)
    gain = lax.dynamic_slice_in_dim(norm_gains[3:4], tp * half, half, 1)
    last = lax.reduce_precision(down.astype(F32) * inverse * gain, 8, 7)
    return (middle.astype(F32) + last).astype(BF16)


def solution(mesh):
    finer = Mesh(
        mesh.devices.reshape(mesh.shape["rep"], 2, 4, 4, mesh.shape["tp"]),
        ("rep", "fs_0", "fs_1", "fs_2", "tp"),
    )
    in_specs = (
        P(REP_FS, "tp"),
        P(),
        P(FS, "tp"),
        P("tp", FS),
        P("tp", FS, None),
        P("tp", FS),
        P(FS, "tp"),
        P("tp", FS),
        P("tp", FS),
        P("tp", FS),
    )
    out_specs = P(REP_FS, "tp")
    return jax.shard_map(
        on_device, mesh=finer, in_specs=in_specs, out_specs=out_specs, check_vma=False
    )
```

```python
import functools
import jax
import jax.numpy as jnp
from jax import lax
from jax.experimental import pallas as pl
from jax.experimental.pallas import tpu as pltpu
from jax.sharding import Mesh
from jax.sharding import PartitionSpec as P


FS = ("fs_0", "fs_1", "fs_2")
REP_FS = ("rep", "fs_0", "fs_1", "fs_2")
EVERY = REP_FS + ("tp",)

EPS = 1e-06
F32, BF16 = jnp.float32, jnp.bfloat16
MIB = 1 << 20

PAIRING = (1, 3, 4, 12, 16, 48)

MIX_ORDERS = ((0, 2, 4, 1, 3), (2, 0, 5, 3, 1), (1, 3, 2, 0, 4), (3, 1, 0, 2, 5))
UP_ORDERS = ((0, 4, 3, 2, 1), (2, 5, 1, 0, 3), (1, 2, 0, 3, 4), (3, 0, 2, 1, 5))
SCALE_ORDER = (0, 2, 4, 1, 3)


def swap_tp(x):
    return lax.ppermute(x, "tp", [(0, 1), (1, 0)])


def swap_with(x, way):
    return lax.ppermute(x, REP_FS, [(i, i ^ PAIRING[way]) for i in range(64)])


def join_kernel(n, added, *refs):
    ins, outs = refs[: 2 * n + 2 * added], refs[2 * n + 2 * added :]
    for k in range(n):
        rows = ins[2 * k].shape[0]
        outs[k][:rows, :] = ins[2 * k][...]
        outs[k][rows:, :] = ins[2 * k + 1][...]
    if added:
        outs[n][...] = ins[2 * n][...] + ins[2 * n + 1][...]


def joined(pairs, added=()):
    outs = [shape(2 * a.shape[0], a.shape[1]) for a, _ in pairs]
    args = [x for pair in pairs for x in pair] + list(added)
    if added:
        outs.append(shape(*added[0].shape, dtype=F32))
    return call(
        functools.partial(join_kernel, len(pairs), len(added) // 2),
        tuple(outs),
        [VMEM] * len(args),
        [],
        12,
        10**6,
    )(*args)


def source_mask(order, place):
    mask = 0
    for k, way in enumerate(order):
        if (place >> k) & 1:
            mask ^= PAIRING[way] & 31
    return mask


def pieces_of(refs, order, rows):
    half = 1 << (len(order) - 1)
    for place in range(2 * half):
        ref = refs[0] if place < half else refs[1]
        yield ref, (place % half) * rows, source_mask(order, place)


def prepare_kernel(where, *refs):
    n = len(MIX_ORDERS)
    ins, outs, held, sems = refs[:7], refs[7:16], refs[16:23], refs[23]
    copies = [pltpu.make_async_copy(x, y, sems.at[k]) for k, (x, y) in enumerate(zip(ins, held))]
    for copy in copies:
        copy.start()
    for copy in copies:
        copy.wait()
    mix, group, up, mix_s, group_s, up_s, down_s = held
    for j in range(n):
        outs[j][:64, :] = mix[:, j * 256 : (j + 1) * 256].astype(BF16)
        outs[j][64:, :] = group[j // 2, :, (j % 2) * 256 : (j % 2) * 256 + 256].astype(BF16)
    for j in range(len(UP_ORDERS)):
        outs[n + j][...] = up[:, j * 512 : (j + 1) * 512].astype(BF16)
    spread = outs[-1]
    row = 0
    for ref in (mix_s, group_s, up_s, down_s):
        count = ref.shape[1]
        place = lax.broadcasted_iota(jnp.int32, (count // 2, count), 0) * 2
        lane = lax.broadcasted_iota(jnp.int32, (count // 2, count), 1)
        column = lax.broadcasted_iota(jnp.int32, (count // 2, 128), 1)
        total = jnp.zeros((count // 2, 128), F32)
        for m in range(2):
            for c in range(2):
                own = jnp.where(lane == place + m, ref[c : c + 1, :], 0.0)
                own = jnp.sum(own, axis=1, keepdims=True)
                total = jnp.where(column == m * 64 + where[0] * 2 + c, own, total)
        spread[row : row + count // 2, :] = total
        row += count // 2


def down_part_kernel(where, down, out, held, sem):
    at = pl.multiple_of(where[2] * 1024, 1024)
    copy = pltpu.make_async_copy(down.at[:, pl.ds(at, 1024)], held, sem)
    copy.start()
    copy.wait()
    out[...] = held[...].astype(BF16)


def own_gain(gains, which, where, k):
    at = pl.multiple_of((where[1] ^ k) * 1024, 1024)
    return gains[which : which + 1, pl.ds(at, 1024)]


def columns(scales, start, count):
    return jnp.concatenate([scales[r : r + 1, :] for r in range(start, start + count)], axis=1)


def first_norm_kernel(where, tok_a, tok_b, gains, normed):
    rows = 128
    gain_a, gain_b = own_gain(gains, 0, where, 0), own_gain(gains, 0, where, 1)

    @pl.loop(0, 1024 // rows)
    def _(b):
        r = pl.ds(pl.multiple_of(b * rows, rows), rows)
        x, y = tok_a[r, :].astype(F32), tok_b[r, :].astype(F32)
        square = jnp.sum(x * x, axis=1, keepdims=True) + jnp.sum(y * y, axis=1, keepdims=True)
        inverse = lax.rsqrt(square * (1.0 / 2048) + EPS)
        normed[r, :1024] = (x * inverse * gain_a).astype(BF16)
        normed[r, 1024:] = (y * inverse * gain_b).astype(BF16)


def mix_kernel(where, normed, scales, *refs):
    n = len(MIX_ORDERS)
    chunks, (out, w, g, m) = refs[: 2 * n], refs[2 * n :]
    fs, tp = where[0], where[1]
    for j, order in enumerate(MIX_ORDERS):
        for ref, row, mask in pieces_of(chunks[2 * j : 2 * j + 2], order, 80):
            at = pl.multiple_of((fs ^ (tp * 16) ^ mask) * 64, 64)
            w[pl.ds(at, 64), j * 256 : (j + 1) * 256] = ref[row : row + 64, :]
            at = pl.multiple_of((fs ^ mask) * 16, 16)
            cols = slice((j % 2) * 256, (j % 2) * 256 + 256)
            g[j // 2, pl.ds(at, 16), cols] = ref[row + 64 : row + 80, :]
    m[0:16, :] = jnp.zeros((16, 1024), F32)
    rows = 256
    for b in range(1024 // rows):
        left = normed[b * rows : (b + 1) * rows, :]
        for k in range(2):
            cols = slice(k * 512, (k + 1) * 512)
            mixed = jnp.dot(left, w[:, cols], preferred_element_type=F32)
            mixed = (mixed * columns(scales, 4 * k, 4)).astype(BF16).astype(F32)
            m[16 + b * rows : 16 + (b + 1) * rows, cols] = mixed
            x = m[b * rows : 16 + (b + 1) * rows, cols]
            two = x + pltpu.roll(x, 1, 0)
            four = two + pltpu.roll(two, 2, 0)
            eight = four + pltpu.roll(four, 4, 0)
            if k == 0:
                sums = jnp.where(tp == 0, two, eight)
                window = jnp.where(tp == 0, 2, 8)
            else:
                sums = jnp.where(tp == 0, four, eight + pltpu.roll(eight, 8, 0))
                window = jnp.where(tp == 0, 4, 16)
            t = lax.broadcasted_iota(jnp.int32, (rows, 1), 0) + (b * rows + 1)
            count = jnp.minimum(t, window).astype(F32)
            pooled = (sums[16:] * (1.0 / count) - mixed).astype(BF16)
            grouped = jnp.dot(pooled, g[k], preferred_element_type=F32)
            out[b * rows : (b + 1) * rows, cols] = (grouped * columns(scales, 8 + 4 * k, 4)).astype(BF16)


def middle_kernel(where, tok_a, tok_b, br_a, br_b, gains, mid, normed):
    rows = 128
    one_a, one_b = own_gain(gains, 1, where, 0), own_gain(gains, 1, where, 1)
    two_a, two_b = own_gain(gains, 2, where, 0), own_gain(gains, 2, where, 1)

    @pl.loop(0, 1024 // rows)
    def _(b):
        r = pl.ds(pl.multiple_of(b * rows, rows), rows)
        x, y = br_a[r, :].astype(F32), br_b[r, :].astype(F32)
        square = jnp.sum(x * x, axis=1, keepdims=True) + jnp.sum(y * y, axis=1, keepdims=True)
        inverse = lax.rsqrt(square * (1.0 / 2048) + EPS)
        x = (x * inverse * one_a).astype(BF16).astype(F32)
        y = (y * inverse * one_b).astype(BF16).astype(F32)
        x = (tok_a[r, :].astype(F32) + x).astype(BF16)
        y = (tok_b[r, :].astype(F32) + y).astype(BF16)
        mid[r, :] = x
        x, y = x.astype(F32), y.astype(F32)
        square = jnp.sum(x * x, axis=1, keepdims=True) + jnp.sum(y * y, axis=1, keepdims=True)
        inverse = lax.rsqrt(square * (1.0 / 2048) + EPS)
        normed[r, :1024] = (x * inverse * two_a).astype(BF16)
        normed[r, 1024:] = (y * inverse * two_b).astype(BF16)


def up_kernel(first, where, normed, scales, *refs):
    orders = UP_ORDERS[first : first + 2]
    chunks, (out, w) = refs[:4], refs[4:]
    fs, tp = where[0], where[1]
    rows = 256
    for j, order in enumerate(orders):
        for ref, row, mask in pieces_of(chunks[2 * j : 2 * j + 2], order, 64):
            at = pl.multiple_of((fs ^ (tp * 16) ^ mask) * 64, 64)
            w[j, pl.ds(at, 64), :] = ref[row : row + 64, :]
        for b in range(1024 // rows):
            r = slice(b * rows, (b + 1) * rows)
            upward = jnp.dot(normed[r, :], w[j], preferred_element_type=F32)
            active = jnp.maximum(upward * columns(scales, 16 + 4 * (first + j), 4), 0.0)
            out[r, j * 512 : (j + 1) * 512] = (active * active).astype(BF16)


NT = (((1,), (1,)), ((), ()))


def down_kernel(where, a0, a1, b0, b1, scales, both, out, square, w, sems):
    tp = where[1]
    for i in sorted(range(64), key=lambda i: (i >> 3) & 1):
        n = i & 15
        pltpu.make_async_copy(
            both.at[pl.ds(i * 64, 64), :],
            w.at[n >> 3, ((i >> 4) & 1) ^ tp, i >> 5, pl.ds((n & 7) * 64, 64), :],
            sems.at[n >> 3],
        ).start()
    rows = 256
    for k in range(2):
        pltpu.make_async_copy(w.at[k], w.at[k], sems.at[k]).wait()
        cols = slice(k * 512, (k + 1) * 512)
        for b in range(1024 // rows):
            r = slice(b * rows, (b + 1) * rows)
            total = lax.dot_general(a0[r, :], w[k, 0, 0], NT, preferred_element_type=F32)
            total += lax.dot_general(a1[r, :], w[k, 0, 1], NT, preferred_element_type=F32)
            total += lax.dot_general(b0[r, :], w[k, 1, 0], NT, preferred_element_type=F32)
            total += lax.dot_general(b1[r, :], w[k, 1, 1], NT, preferred_element_type=F32)
            down = (total * columns(scales, 32 + 4 * k, 4)).astype(BF16)
            out[r, cols] = down
            down = down.astype(F32)
            squares = jnp.sum(down * down, axis=1, keepdims=True)
            if k == 0:
                square[r, :] = squares
            else:
                square[r, :] += squares


SMEM = pl.BlockSpec(memory_space=pltpu.SMEM)
VMEM = pl.BlockSpec(memory_space=pltpu.VMEM)
ANY = pl.BlockSpec(memory_space=pl.ANY)


def call(kernel, out_shape, in_specs, scratch, limit, flops):
    multiple = isinstance(out_shape, tuple)
    return pl.pallas_call(
        kernel,
        out_shape=out_shape,
        in_specs=in_specs,
        out_specs=(VMEM,) * len(out_shape) if multiple else VMEM,
        scratch_shapes=scratch,
        compiler_params=pltpu.CompilerParams(vmem_limit_bytes=limit * MIB),
        cost_estimate=pl.CostEstimate(flops=flops, bytes_accessed=16 * MIB, transcendentals=0),
    )


def shape(*dims, dtype=BF16):
    return jax.ShapeDtypeStruct(dims, dtype)


def on_device(
    tokens,
    norm_gains,
    mix_weight,
    mix_scale,
    group_weight,
    group_scale,
    up_weight,
    up_scale,
    down_weight,
    down_scale,
):
    tp = lax.axis_index("tp")
    where = jnp.stack([lax.axis_index(FS), tp, lax.axis_index("rep")]).astype(jnp.int32)
    half = 1024

    down = call(
        down_part_kernel,
        shape(64, half),
        [SMEM, ANY],
        [pltpu.VMEM((64, 1024), F32), pltpu.SemaphoreType.DMA],
        58,
        10**6,
    )(where, jnp.transpose(down_weight))
    trade = []
    for i in range(64):
        for c in range(2):
            trade.append((i * 2 + c, i * 2 + c if (i >> 4) & 1 == c else (i ^ 16) * 2 + 1 - c))
    down = lax.ppermute(down, EVERY, trade)
    down = lax.all_gather(down, REP_FS, axis=0, tiled=True)

    *parts, scales = call(
        prepare_kernel,
        (shape(80, 256),) * 4 + (shape(64, 512),) * 4 + (shape(40, 128, dtype=F32),),
        [SMEM] + [ANY] * 7,
        [
            pltpu.VMEM((64, 1024), F32),
            pltpu.VMEM((2, 16, 512), F32),
            pltpu.VMEM((64, 2048), F32),
            pltpu.VMEM((2, 16), F32),
            pltpu.VMEM((2, 16), F32),
            pltpu.VMEM((2, 32), F32),
            pltpu.VMEM((2, 16), F32),
            pltpu.SemaphoreType.DMA((7,)),
        ],
        58,
        10**6,
    )(
        where,
        mix_weight,
        group_weight,
        up_weight,
        *(jnp.transpose(x) for x in (mix_scale, group_scale, up_scale, down_scale)),
    )
    mix_held, up_held = parts[:4], parts[4:]

    def step(held, orders, k):
        return [(x, swap_with(x, order[k])) for x, order in zip(held, orders)]

    for k in range(5):
        pairs = step(mix_held, MIX_ORDERS, k)
        sent = swap_with(scales, SCALE_ORDER[k])
        if k < 4:
            *mix_held, scales = joined(pairs, (scales, sent))
        if k == 0:
            tokens_late, _ = lax.optimization_barrier((tokens, scales))
            other = swap_tp(tokens_late)
    scales = scales + sent
    mix_parts = [x for pair in pairs for x in pair]
    for k in range(5):
        pairs = step(up_held, UP_ORDERS, k)
        if k < 4:
            up_held = joined(pairs)
    up_parts = [x for pair in pairs for x in pair]

    normed = call(
        first_norm_kernel, shape(1024, 2 * half), [SMEM] + [VMEM] * 3, [], 16, 10**9
    )(where, tokens, other, norm_gains)

    branch = call(
        mix_kernel,
        shape(1024, half),
        [SMEM, VMEM, VMEM] + [VMEM] * len(mix_parts),
        [
            pltpu.VMEM((2048, 1024), BF16),
            pltpu.VMEM((2, 512, 512), BF16),
            pltpu.VMEM((1040, 1024), F32),
        ],
        24,
        6 * 10**9,
    )(where, normed, scales, *mix_parts)

    middle, normed_mid = call(
        middle_kernel,
        (shape(1024, half), shape(1024, 2 * half)),
        [SMEM] + [VMEM] * 5,
        [],
        20,
        10**9,
    )(where, tokens, other, branch, swap_tp(branch), norm_gains)

    hidden = []
    for first in (0, 2):
        hidden.append(
            call(
                functools.partial(up_kernel, first),
                shape(1024, 1024),
                [SMEM] + [VMEM] * 6,
                [pltpu.VMEM((2, 2048, 512), BF16)],
                16,
                5 * 10**9,
            )(where, normed_mid, scales, *up_parts[2 * first : 2 * first + 4])
        )

    down, square = call(
        down_kernel,
        (shape(1024, half), shape(1024, 1, dtype=F32)),
        [SMEM] + [VMEM] * 5 + [ANY],
        [pltpu.VMEM((2, 2, 2, 512, 1024), BF16), pltpu.SemaphoreType.DMA((2,))],
        36,
        9 * 10**9,
    )(where, *hidden, *(swap_tp(x) for x in hidden), scales, down)

    inverse = lax.rsqrt((square + swap_tp(square)) / (2 * half) + EPS)
    gain = lax.dynamic_slice_in_dim(norm_gains[3:4], tp * half, half, 1)
    last = lax.reduce_precision(down.astype(F32) * inverse * gain, 8, 7)
    return (middle.astype(F32) + last).astype(BF16)


def solution(mesh):
    finer = Mesh(
        mesh.devices.reshape(mesh.shape["rep"], 2, 4, 4, mesh.shape["tp"]),
        ("rep", "fs_0", "fs_1", "fs_2", "tp"),
    )
    in_specs = (
        P(REP_FS, "tp"),
        P(),
        P(FS, "tp"),
        P("tp", FS),
        P("tp", FS, None),
        P("tp", FS),
        P(FS, "tp"),
        P("tp", FS),
        P("tp", FS),
        P("tp", FS),
    )
    out_specs = P(REP_FS, "tp")
    return jax.shard_map(
        on_device, mesh=finer, in_specs=in_specs, out_specs=out_specs, check_vma=False
    )
```
